128 devices in a mesh: ep: 32 (over z, y, core), tp: 4 (over x).
Axes of the slice: x: 4, y: 4, z: 4, core: 2. Of those that a mesh axis runs over, the one named last changes fastest.
Arguments:
- q_latent: bfloat16 [16384, 512], P(('ep', 'tp')), may hold values from -6 to 6
- kv_latent: bfloat16 [16384, 256], P(('ep', 'tp')), may hold values from -6 to 6
- rope_key: bfloat16 [16384, 32], P(('ep', 'tp')), may hold values from -240 to 240
- q_gain: float32 [512], replicated, may hold values from 0.1 to 1.9
- kv_gain: float32 [256], replicated, may hold values from 0.1 to 1.9
- w_query: bfloat16 [512, 1024], P(None, 'tp'), may hold values from -0.25 to 0.25
- w_query_rot: bfloat16 [512, 512], P(None, 'tp'), may hold values from -0.25 to 0.25
- w_key: bfloat16 [256, 1024], P(None, 'tp'), may hold values from -0.375 to 0.375
- w_value: bfloat16 [256, 1024], P(None, 'tp'), may hold values from -0.375 to 0.375
- w_mix_out: bfloat16 [1024, 2048], P('tp'), may hold values from -0.1875 to 0.1875
- expert_input: bfloat16 [16384, 2048], P(('ep', 'tp')), may hold values from -6 to 6
- ffn_gain: float32 [2048], replicated, may hold values from 0.1 to 1.9
- expert_ids: int32 [16384, 4], P(('ep', 'tp')), may hold values from 0 to 31, all different within a row; in each aligned block of 128 rows (0 to 127, 128 to 255, ...) at most 24 rows name the same one
- route_weights: float32 [16384, 4], P(('ep', 'tp')), may hold values from 0.2 to 1
- w_gate_exp: bfloat16 [32, 2048, 1024], P('ep', None, 'tp'), may hold values from -0.125 to 0.125
- w_up_exp: bfloat16 [32, 2048, 1024], P('ep', None, 'tp'), may hold values from -0.125 to 0.125
- w_down_exp: bfloat16 [32, 1024, 2048], P('ep', 'tp'), may hold values from -0.1875 to 0.1875
Outputs:
- mixer_out: bfloat16 [16384, 2048], P(('ep', 'tp'))
- expert_out: bfloat16 [16384, 2048], P(('ep', 'tp'))
The draws below stay inside these ranges and needn't reach their ends.
Inputs may be any that keep to these rules, and one draw needn't show every extreme that they name: `expert_ids`: the experts of a row are all different. In the rows of one device (aligned blocks of 128 tokens) no expert is named by more than 24 rows, a bound that some block reaches.
All inputs are finite; a program needn't handle non-finite values.
Results may differ from the reference program's by a relative error of at most 0.012.
The reference program's roundings to bfloat16 on the way count: a program that leaves them out, or rounds other values in their place, can miss the bound.
Values may be sent and summed in bfloat16 or wider, within the bound.
No kernel may reach another device: no remote copies, remote signals or barrier semaphores. Data moves between devices by JAX's collectives and lax.ppermute only.
A program may use at most 128 MiB of HBM per device.

```python
import math
import jax
import jax.numpy as jnp
import numpy as np
from jax import lax

D = 2048
HEADS = 16
NOPE = 64
ROPE = 32
VD = 64
Q_RANK = 512
KV_RANK = 256
FF = 1024
TOPK = 4
SEG = 64
TOK_DEV = 128
EXPERTS = 32
TOKENS = 16384
CAP = 24
N_EP = 32
N_TP = 4


def draw_rope_key(key, part):
    drawn = jnp.clip(jax.random.normal(jax.random.fold_in(key, 11), (TOKENS, ROPE), jnp.float32), -6.0, 6.0)
    return drawn.astype(jnp.bfloat16)


def levels(key, dims, split, least, high):
    loudness = 1.0
    for position, blocks in split:
        steps = jax.random.uniform(jax.random.fold_in(jax.random.fold_in(key, 6), position), (blocks,), jnp.float32, least / len(split), high / len(split))
        loudness = loudness * jnp.repeat(jnp.exp(steps), dims[position] // blocks).reshape((-1,) + (1,) * (len(dims) - 1 - position))
    return loudness


def deal_out(key, own, number, rows, number_of, top, bound, skew):
    order = jax.random.permutation(key, number_of)
    packed, ordinary = shares(number_of, rows * top, bound, skew, True), shares(number_of, rows * top, bound, skew, False)
    places = jnp.arange(number_of)

    def named(tallies, offset_by):
        used = int((tallies > 0).sum())
        fixed = max(1, used // 4)
        moved = fixed + (places - fixed + offset_by * (used - fixed)) % max(1, number_of - fixed)
        return jnp.zeros((number_of,), jnp.int32).at[order[jnp.where(places < fixed, places, moved)]].set(jnp.asarray(tallies, jnp.int32))

    tallies = jnp.where(number % 4 == 0, named(packed, number // 4), named(ordinary, number - number // 4 - 1))
    mixed = jax.random.permutation(jax.random.fold_in(own, 3), number_of)
    giver, taker = mixed[0:number_of // 2 * 2:2], mixed[1:number_of // 2 * 2:2]
    slack = jnp.minimum(tallies[giver] - 1, bound - tallies[taker]) // 2
    slack = jnp.where((giver == order[0]) | (taker == order[0]) | (tallies[taker] == 0), 0, jnp.maximum(slack, 0))
    moved = jax.random.randint(jax.random.fold_in(own, 4), (number_of // 2,), 0, 1 << 20) % (slack + 1)
    tallies = tallies.at[giver].add(-moved).at[taker].add(moved)
    members = jnp.searchsorted(jnp.cumsum(tallies), jnp.arange(rows * top), side="right").astype(jnp.int32)
    grid = members.reshape(top, rows).T
    grid = grid[jax.random.permutation(jax.random.fold_in(own, 1), rows)]
    offset_by = jax.random.randint(jax.random.fold_in(own, 2), (rows, 1), 0, top)
    return jnp.take_along_axis(grid, (jnp.arange(top)[None, :] + offset_by) % top, axis=1)


def shares(amount, total, limit, lean, full):
    weights = [(1 << 20) // math.isqrt(rank ** lean) + 1 for rank in range(1, amount + 1)]
    largest = limit if full else min(limit, max(-(-total // amount), total * weights[0] // sum(weights)))
    least = 1 if total - largest >= amount - 1 else 0
    holding, surplus = [largest] + [least] * (amount - 1), total - largest - least * (amount - 1)
    while surplus > 0:
        free = [i for i in range(1, amount) if holding[i] < largest] or [i for i in range(1, amount) if holding[i] < limit]
        whole, budget = sum([weights[i] for i in free]), surplus
        for i in free:
            more = min(limit - holding[i], max(1, budget * weights[i] // whole), surplus)
            holding[i] = holding[i] + more
            surplus = surplus - more
    return np.array(holding)


def noise(key, dims, width, limit, split=(), kind=jnp.bfloat16):
    result = width * jax.random.normal(key, dims, jnp.float32)
    if split:
        result = result * levels(key, dims, split, -0.22, 0.18)
    return jnp.clip(result, -limit, limit).astype(kind)


def setup_inputs(seed: int = 0) -> dict:
    keys = jax.random.split(jax.random.key(seed), 18)
    q_latent = noise(keys[0], (TOKENS, Q_RANK), 1.0, 6.0, ((0, 128),))
    kv_latent = noise(keys[1], (TOKENS, KV_RANK), 1.0, 6.0, ((0, 128),))
    rope_key = draw_rope_key(jax.random.fold_in(keys[17], 71), 0)
    q_gain = jnp.clip(1.0 + 0.18 * jax.random.normal(keys[3], (Q_RANK,), jnp.float32), 0.1, 1.9)
    kv_gain = jnp.clip(1.0 + 0.18 * jax.random.normal(keys[4], (KV_RANK,), jnp.float32), 0.1, 1.9)
    w_query = noise(keys[5], (Q_RANK, HEADS * NOPE), Q_RANK ** -0.5, 0.25, ((1, 4),))
    w_query_rot = noise(keys[6], (Q_RANK, HEADS * ROPE), Q_RANK ** -0.5, 0.25, ((1, 4),))
    w_key = noise(keys[7], (KV_RANK, HEADS * NOPE), KV_RANK ** -0.5, 0.375, ((1, 4),))
    w_value = noise(keys[8], (KV_RANK, HEADS * VD), KV_RANK ** -0.5, 0.375, ((1, 4),))
    w_mix_out = noise(keys[9], (HEADS * VD, D), (HEADS * VD) ** -0.5, 0.1875, ((0, 4),))
    expert_input = noise(keys[10], (TOKENS, D), 1.0, 6.0, ((0, 128),))
    ffn_gain = jnp.clip(1.0 + 0.18 * jax.random.normal(keys[11], (D,), jnp.float32), 0.1, 1.9)
    expert_ids_keys = jax.random.split(jax.random.fold_in(keys[12], 1), TOKENS // TOK_DEV)
    expert_ids_turns = jax.random.permutation(jax.random.fold_in(keys[12], 3), TOKENS // TOK_DEV)
    expert_ids = jax.vmap(lambda own, number: deal_out(jax.random.fold_in(keys[12], 2), own, number, TOK_DEV, EXPERTS, TOPK, CAP, 2))(expert_ids_keys, expert_ids_turns).reshape((TOKENS, TOPK))
    route_weights = jnp.clip(0.2 + 0.8 * jax.random.uniform(keys[13], (TOKENS, TOPK), jnp.float32) ** levels(keys[13], (TOKENS, TOPK), ((0, 128),), -0.2, 0.2), 0.2, 1.0)
    w_gate_exp = noise(keys[14], (EXPERTS, D, FF), D ** -0.5, 0.125, ((0, 32), (2, 4)))
    w_up_exp = noise(keys[15], (EXPERTS, D, FF), D ** -0.5, 0.125, ((0, 32), (2, 4)))
    w_down_exp = noise(keys[16], (EXPERTS, FF, D), FF ** -0.5, 0.1875, ((0, 32), (1, 4)))
    return dict(q_latent=q_latent, kv_latent=kv_latent, rope_key=rope_key, q_gain=q_gain, kv_gain=kv_gain, w_query=w_query, w_query_rot=w_query_rot, w_key=w_key, w_value=w_value, w_mix_out=w_mix_out, expert_input=expert_input, ffn_gain=ffn_gain, expert_ids=expert_ids, route_weights=route_weights, w_gate_exp=w_gate_exp, w_up_exp=w_up_exp, w_down_exp=w_down_exp)


norm_epsilon = 1e-06
rope_base = 10000.0
query_block = 256

def rms_scale(values_in, gain_vec):
    floats = values_in.astype(jnp.float32)
    return floats * lax.rsqrt(lax.optimization_barrier(jnp.mean(floats * floats, axis=-1, keepdims=True)) + norm_epsilon) * gain_vec

def tables(positions):
    half_width = ROPE // 2
    frequency = rope_base ** (-jnp.arange(half_width, dtype=jnp.float32) / half_width)
    angles = positions.astype(jnp.float32)[:, None] * frequency[None, :]
    return (jnp.cos(angles), jnp.sin(angles))

def rotate_pairs(values_in, cosine, sine_table):
    half_width = values_in.shape[-1] // 2
    first, second = (values_in[..., :half_width], values_in[..., half_width:])
    return jnp.concatenate([first * cosine - second * sine_table, first * sine_table + second * cosine], axis=-1)

def mixer(q_latent, kv_latent, rope_key, q_gain, kv_gain, w_query, w_query_rot, w_key, w_value, w_mix_out):
    row_total = q_latent.shape[0]
    positions = jnp.arange(row_total, dtype=jnp.int32)
    cosine, sine_table = tables(positions)
    q_normed = rms_scale(q_latent, q_gain).astype(jnp.bfloat16)
    q_plain = jnp.dot(q_normed, w_query, preferred_element_type=jnp.float32).astype(jnp.bfloat16)
    q_plain = q_plain.reshape(row_total, HEADS, NOPE)
    q_turned = jnp.dot(q_normed, w_query_rot, preferred_element_type=jnp.float32).reshape(row_total, HEADS, ROPE)
    q_turned = rotate_pairs(q_turned, cosine[:, None, :], sine_table[:, None, :]).astype(jnp.bfloat16)
    kv_normed = rms_scale(kv_latent, kv_gain).astype(jnp.bfloat16)
    k_plain = jnp.dot(kv_normed, w_key, preferred_element_type=jnp.float32).astype(jnp.bfloat16)
    k_plain = k_plain.reshape(row_total, HEADS, NOPE).astype(jnp.float32)
    values = jnp.dot(kv_normed, w_value, preferred_element_type=jnp.float32).astype(jnp.bfloat16)
    values = values.reshape(row_total, HEADS, VD).astype(jnp.float32)
    k_turned = rotate_pairs(rope_key.astype(jnp.float32), cosine, sine_table).astype(jnp.bfloat16).astype(jnp.float32)
    segment = positions // SEG
    score_scale = (NOPE + ROPE) ** (-0.5)

    def attend(first_row):
        block_plain = lax.dynamic_slice_in_dim(q_plain, first_row, query_block, 0).astype(jnp.float32)
        block_turned = lax.dynamic_slice_in_dim(q_turned, first_row, query_block, 0).astype(jnp.float32)
        scores = jnp.einsum('qhd,khd->hqk', block_plain, k_plain) + jnp.einsum('qhd,kd->hqk', block_turned, k_turned)
        scores = scores * score_scale
        query_segment = (first_row + jnp.arange(query_block, dtype=jnp.int32)) // SEG
        allowed = segment[None, :] <= query_segment[:, None]
        scores = jnp.where(allowed[None], scores, -jnp.inf)
        row_max = lax.optimization_barrier(jnp.max(scores, axis=-1, keepdims=True))
        weights = jnp.where(allowed[None], jnp.exp(scores - row_max), 0.0)
        weight_sum = lax.optimization_barrier(jnp.sum(weights, axis=-1))
        rounded = weights.astype(jnp.bfloat16).astype(jnp.float32)
        mixed = jnp.einsum('hqk,khd->qhd', rounded, values) / jnp.transpose(weight_sum)[:, :, None]
        return mixed.astype(jnp.bfloat16).reshape(query_block, HEADS * VD)
    starts = jnp.arange(0, row_total, query_block, dtype=jnp.int32)
    attention = lax.map(attend, starts).reshape(row_total, HEADS * VD)
    block_width = HEADS * VD // N_TP
    summed = jnp.zeros((row_total, D), jnp.float32)
    for block_index in range(N_TP):
        columns = attention[:, block_index * block_width:(block_index + 1) * block_width]
        weight_rows = w_mix_out[block_index * block_width:(block_index + 1) * block_width]
        partial_out = jnp.dot(columns, weight_rows, preferred_element_type=jnp.float32).astype(jnp.bfloat16)
        summed = summed + lax.optimization_barrier(partial_out).astype(jnp.float32)
    return summed.astype(jnp.bfloat16)

def experts(expert_input, ffn_gain, expert_ids, route_weights, w_gate_exp, w_up_exp, w_down_exp):
    row_total = expert_input.shape[0]
    groups = N_EP * N_TP
    expert_count = w_gate_exp.shape[0]
    normed = rms_scale(expert_input, ffn_gain).astype(jnp.bfloat16)
    routed = expert_ids.reshape(groups, TOK_DEV * TOPK).astype(jnp.int32)
    onehot = (routed[:, :, None] == jnp.arange(expert_count, dtype=jnp.int32)[None, None, :]).astype(jnp.int32)
    slot_number = lax.optimization_barrier(jnp.sum((jnp.cumsum(onehot, axis=1) - 1) * onehot, axis=-1)).astype(jnp.int32)
    group_index = jnp.arange(groups, dtype=jnp.int32)[:, None]
    slot_place = ((routed * groups + group_index) * CAP + slot_number).reshape(-1).astype(jnp.int32)
    token_index = group_index * TOK_DEV + jnp.arange(TOK_DEV * TOPK, dtype=jnp.int32)[None, :] // TOPK
    token_table = jnp.zeros((expert_count * groups * CAP,), jnp.int32).at[slot_place].set(token_index.reshape(-1).astype(jnp.int32))
    token_table = token_table.reshape(expert_count, groups * CAP)
    block_width = FF // N_TP

    def expert_block(arguments):
        rows_idx, gate_weight, up_weight, down_weight = arguments
        chosen = normed[rows_idx]
        gate_part = jnp.dot(chosen, gate_weight, preferred_element_type=jnp.float32)
        up_part = jnp.dot(chosen, up_weight, preferred_element_type=jnp.float32)
        hidden = (jax.nn.silu(gate_part) * up_part).astype(jnp.bfloat16)
        summed = jnp.zeros((chosen.shape[0], D), jnp.float32)
        for block_index in range(N_TP):
            columns = hidden[:, block_index * block_width:(block_index + 1) * block_width]
            weight_rows = down_weight[block_index * block_width:(block_index + 1) * block_width]
            partial_out = jnp.dot(columns, weight_rows, preferred_element_type=jnp.float32).astype(jnp.bfloat16)
            summed = summed + lax.optimization_barrier(partial_out).astype(jnp.float32)
        return summed.astype(jnp.bfloat16)
    results = lax.map(expert_block, (token_table, w_gate_exp, w_up_exp, w_down_exp))
    all_results = results.reshape(-1, D)
    picked = all_results[slot_place].astype(jnp.float32).reshape(row_total, TOPK, D)
    weighted_sum = lax.optimization_barrier(jnp.sum(picked * route_weights[:, :, None].astype(jnp.float32), axis=1))
    return weighted_sum.astype(jnp.bfloat16)

def reference(q_latent, kv_latent, rope_key, q_gain, kv_gain, w_query, w_query_rot, w_key, w_value, w_mix_out, expert_input, ffn_gain, expert_ids, route_weights, w_gate_exp, w_up_exp, w_down_exp):
    mixer_out = mixer(q_latent, kv_latent, rope_key, q_gain, kv_gain, w_query, w_query_rot, w_key, w_value, w_mix_out)
    expert_out = experts(expert_input, ffn_gain, expert_ids, route_weights, w_gate_exp, w_up_exp, w_down_exp)
    return (mixer_out, expert_out)
```

```python
import math

import jax
import jax.numpy as jnp
from jax import lax
from jax.experimental import pallas as pl
from jax.experimental.pallas import tpu as pltpu
from jax.sharding import PartitionSpec as P


D = 2048
NOPE = 64
ROPE = 32
TOPK = 4

norm_epsilon = 1e-06
rope_base = 10000.0
masked_score = -1e30


KEYS = 512
QUERIES = 256
HEADS_HERE = 4
STEPS_A_CHUNK = 4
PIECE = 256
excess_limit = 60.0
exponent_scale = (NOPE + ROPE) ** (-0.5) * math.log2(math.e)

BY_LAST = (((1,), (1,)), ((), ()))
BY_FIRST = (((0,), (0,)), ((), ()))


def rms_scale(values_in, gain_vec):
    floats = values_in.astype(jnp.float32)
    return (
        floats
        * lax.rsqrt(jnp.mean(floats * floats, axis=-1, keepdims=True) + norm_epsilon)
        * gain_vec
    )


def tables(positions):
    half_width = ROPE // 2
    frequency = rope_base ** (-jnp.arange(half_width, dtype=jnp.float32) / half_width)
    angles = positions.astype(jnp.float32)[:, None] * frequency[None, :]
    return (jnp.cos(angles), jnp.sin(angles))


def rotate_pairs(values_in, cosine, sine_table):
    half_width = values_in.shape[-1] // 2
    first, second = (values_in[..., :half_width], values_in[..., half_width:])
    return jnp.concatenate(
        [first * cosine - second * sine_table, first * sine_table + second * cosine], axis=-1
    )


def attention_kernel(
    place_ref,
    kv_ref,
    q_ref,
    wq_ref,
    wr_ref,
    cos_ref,
    sin_ref,
    wk_ref,
    wv_ref,
    wo_ref,
    after_ref,
    out_ref,
    held_ref,
    query_ref,
    pair_ref,
    vt_ref,
    max_ref,
    sum_ref,
    excess_ref,
    sem,
):
    group = place_ref[0]
    last = place_ref[1]
    low = 31 - last
    chunk = 4 * STEPS_A_CHUNK
    chunks = 32 // STEPS_A_CHUNK
    copies = [
        pltpu.make_async_copy(
            kv_ref.at[pl.ds(n * chunk, chunk)], held_ref.at[pl.ds(n * chunk, chunk)], sem.at[n]
        )
        for n in range(chunks)
    ]
    for copy in copies:
        copy.start()

    for half in range(2):
        rows = jnp.concatenate(
            [
                jnp.concatenate(
                    [
                        q_ref[half, place_ref[2 + t], n * 64 : n * 64 + 64]
                        for n in range(4)
                    ],
                    axis=1,
                )
                for t in range(4)
            ],
            axis=0,
        )
        plain = lax.dot_general(
            wq_ref[...], rows, BY_LAST, preferred_element_type=jnp.float32
        ).astype(jnp.bfloat16)
        turned = lax.dot_general(wr_ref[...], rows, BY_LAST, preferred_element_type=jnp.float32)
        cosine, sine = cos_ref[half], sin_ref[half]
        for h in range(HEADS_HERE):
            first = turned[h * 32 : h * 32 + 16]
            second = turned[h * 32 + 16 : h * 32 + 32]
            at = (h % 2) * 64
            query_ref[half, h, at : at + 64] = plain[h * 64 : h * 64 + 64]
            query_ref[half, h, 64 - at : 128 - at] = jnp.zeros((64, QUERIES), jnp.bfloat16)
            query_ref[half, h, 128:144] = (first * cosine - second * sine).astype(jnp.bfloat16)
            query_ref[half, h, 144:160] = (first * sine + second * cosine).astype(jnp.bfloat16)
            query_ref[half, h, 160:256] = jnp.zeros((96, QUERIES), jnp.bfloat16)
    for h in range(HEADS_HERE):
        vt_ref[h, 64:80] = jnp.ones((16, KEYS), jnp.bfloat16)

    def clear():
        max_ref[...] = jnp.full_like(max_ref, masked_score)
        sum_ref[...] = jnp.zeros_like(sum_ref)

    def project(j):
        base = j * 4
        normed_rows, rope_rows = [], []
        for t in range(4):
            at = base + place_ref[2 + t]
            normed_rows.append(
                jnp.concatenate([held_ref[at, 0:128], held_ref[at, 128:256]], axis=1)
            )
            packed = held_ref[at, 256:288].astype(jnp.float32)
            for k in range(4):
                rope_rows.append(
                    (packed if k == 0 else pltpu.roll(packed, 128 - 32 * k, 1)).astype(jnp.bfloat16)
                )
        normed = jnp.concatenate(normed_rows, axis=0)
        rope = jnp.concatenate(rope_rows, axis=0)
        keys = jnp.dot(normed, wk_ref[...], preferred_element_type=jnp.float32).astype(jnp.bfloat16)
        vals = lax.dot_general(
            wv_ref[...], normed, BY_LAST, preferred_element_type=jnp.float32
        ).astype(jnp.bfloat16)
        for p in range(2):
            pair_ref[p, :, 0:128] = keys[:, p * 128 : p * 128 + 128]
            pair_ref[p, :, 128:256] = rope
        for h in range(HEADS_HERE):
            vt_ref[h, 0:64] = vals[h * 64 : h * 64 + 64]

    def hidden_keys(j, half):
        edge = jnp.where(half == 0, group, 31 - group)
        key_segment = lax.broadcasted_iota(jnp.int32, (KEYS, QUERIES), 0) // 64 + 8 * j
        query_segment = (
            2 * (lax.broadcasted_iota(jnp.int32, (KEYS, QUERIES), 1) // 64) + half + 8 * edge
        )
        return key_segment > query_segment

    def safe_tile(j, half):
        hidden = hidden_keys(j, half)
        for h in range(HEADS_HERE):
            scores = jnp.dot(
                pair_ref[h // 2], query_ref[half, h], preferred_element_type=jnp.float32
            )
            scores = jnp.where(hidden, masked_score, scores)
            old = max_ref[half, h, 0:1]
            new = jnp.maximum(old, jnp.max(scores, axis=0, keepdims=True))
            factor = jnp.exp2((old - new) * exponent_scale)
            weights = jnp.exp2((scores - new) * exponent_scale).astype(jnp.bfloat16)
            part = jnp.dot(vt_ref[h], weights, preferred_element_type=jnp.float32)
            sum_ref[half, h] = sum_ref[half, h] * factor + part
            max_ref[half, h, 0:1] = new

    def tiles(j, halves, masked):
        units = [(half, h) for half in halves for h in range(HEADS_HERE)]
        hidden = hidden_keys(j, halves[0]) if masked else None
        count = len(units)
        base = [max_ref[half, h, 0:1] for half, h in units]
        peak, weights = [None] * count, [None] * count

        def weigh(u):
            half, h = units[u]
            tops, pieces = [], []
            for p in range(0, KEYS, PIECE):
                scores = jnp.dot(
                    pair_ref[h // 2, p : p + PIECE],
                    query_ref[half, h],
                    preferred_element_type=jnp.float32,
                )
                if masked:
                    scores = jnp.where(hidden[p : p + PIECE], masked_score, scores)
                tops.append(jnp.max(scores, axis=0, keepdims=True))
                pieces.append(
                    jnp.exp2((scores - base[u]) * exponent_scale).astype(jnp.bfloat16)
                )
            top = tops[0]
            for other in tops[1:]:
                top = jnp.maximum(top, other)
            peak[u] = top
            weights[u] = jnp.concatenate(pieces, axis=0)

        def gather(u):
            half, h = units[u]
            part = jnp.dot(vt_ref[h], weights[u], preferred_element_type=jnp.float32)
            new = jnp.maximum(base[u], peak[u])
            factor = jnp.exp2((base[u] - new) * exponent_scale)
            sum_ref[half, h] = (sum_ref[half, h] + part) * factor
            max_ref[half, h, 0:1] = new

        for u in range(count + 1):
            if u < count:
                weigh(u)
            if u:
                gather(u - 1)
        most = peak[0] - base[0]
        for u in range(1, count):
            most = jnp.maximum(most, peak[u] - base[u])
        excess_ref[0:1] = jnp.maximum(excess_ref[0:1], most)

    def safe_step(j):
        project(j)
        for half in range(2):
            edge = group if half == 0 else 31 - group

            @pl.when(j <= edge)
            def _():
                safe_tile(j, half)

    def one_half(j):
        for half in range(2):
            edge = group if half == 0 else 31 - group

            @pl.when(jnp.logical_and(j >= low, j < edge))
            def _():
                tiles(j, (half,), False)

            @pl.when(j == edge)
            def _():
                tiles(j, (half,), True)

    clear()
    excess_ref[...] = jnp.zeros_like(excess_ref)
    copies[0].wait()
    lax.fori_loop(0, 1, lambda j, c: (safe_step(j), c)[1], 0)

    def step(j, carried):
        for n in range(1, chunks):

            @pl.when(j == n * STEPS_A_CHUNK)
            def _():
                copies[n].wait()

        project(j)

        @pl.when(j < low)
        def _():
            tiles(j, (0, 1), False)

        @pl.when(j >= low)
        def _():
            one_half(j)

        return carried

    lax.fori_loop(1, last + 1, step, 0)
    for n in range(1, chunks):

        @pl.when(last < n * STEPS_A_CHUNK)
        def _():
            copies[n].wait()

    worst = jnp.max(excess_ref[0:1]) * exponent_scale

    @pl.when(jnp.logical_not(worst < excess_limit))
    def _():
        clear()
        lax.fori_loop(0, last + 1, lambda j, c: (safe_step(j), c)[1], 0)

    for half in range(2):
        heads = [
            (sum_ref[half, h, 0:64] / sum_ref[half, h, 64:65]).astype(jnp.bfloat16)
            for h in range(HEADS_HERE)
        ]
        attended = jnp.concatenate(heads, axis=0)
        part = lax.dot_general(
            attended, wo_ref[...], BY_FIRST, preferred_element_type=jnp.float32
        ).astype(jnp.bfloat16)
        out_ref[:, half] = part.reshape(4, 64, D)


def attention(place, kv, q, wq_t, wr_t, cosine, sine, wk, wv_t, wo, after):
    return pl.pallas_call(
        attention_kernel,
        in_specs=[
            pl.BlockSpec(memory_space=pltpu.SMEM),
            pl.BlockSpec(memory_space=pl.ANY),
        ]
        + [pl.BlockSpec(memory_space=pltpu.VMEM)] * 8
        + [pl.BlockSpec(memory_space=pl.ANY)],
        out_specs=pl.BlockSpec(memory_space=pltpu.VMEM),
        scratch_shapes=[
            pltpu.VMEM((128, 288, 128), jnp.bfloat16),
            pltpu.VMEM((2, HEADS_HERE, 256, QUERIES), jnp.bfloat16),
            pltpu.VMEM((2, KEYS, 256), jnp.bfloat16),
            pltpu.VMEM((HEADS_HERE, 80, KEYS), jnp.bfloat16),
            pltpu.VMEM((2, HEADS_HERE, 8, QUERIES), jnp.float32),
            pltpu.VMEM((2, HEADS_HERE, 80, QUERIES), jnp.float32),
            pltpu.VMEM((8, QUERIES), jnp.float32),
            pltpu.SemaphoreType.DMA((32 // STEPS_A_CHUNK,)),
        ],
        out_shape=jax.ShapeDtypeStruct((4, 2, 64, D), jnp.bfloat16),
        cost_estimate=pl.CostEstimate(
            flops=30_000_000_000, bytes_accessed=16_000_000, transcendentals=17_000_000
        ),
        name="attention",
    )(place, kv, q, wq_t, wr_t, cosine, sine, wk, wv_t, wo, after)


ROWS = 256
COLUMNS = 512


def experts_kernel(pieces, carried, x_ref, *refs):
    total_pieces = sum(sum(block) for block in pieces)
    parts = refs[:total_pieces]
    refs = refs[total_pieces + 1 :]
    before_ref = None
    if carried:
        before_ref, refs = refs[0], refs[1:]
    out_ref = refs[0]
    held = refs[1 : 1 + 3 * len(pieces)]
    sem = refs[1 + 3 * len(pieces)]
    copies, n = [], 0
    for b, block in enumerate(pieces):
        for role, number in enumerate(block):
            target, own = held[3 * b + role], []
            for piece in range(number):
                rows = target.shape[0] // number
                own.append(
                    pltpu.make_async_copy(
                        parts[n], target.at[pl.ds(piece * rows, rows)], sem.at[n]
                    )
                )
                n += 1
            copies.append(own)
    first_step = pl.program_id(0) == 0

    @pl.when(first_step)
    def _():
        for own in copies:
            for copy in own:
                copy.start()

    def ready(n):
        @pl.when(first_step)
        def _():
            for copy in copies[n]:
                copy.wait()

    rows = x_ref[...]
    hidden = []
    for b in range(len(pieces)):
        ready(3 * b)
        gate_part = jnp.dot(rows, held[3 * b][...], preferred_element_type=jnp.float32)
        ready(3 * b + 1)
        up_part = jnp.dot(rows, held[3 * b + 1][...], preferred_element_type=jnp.float32)
        hidden.append((jax.nn.silu(gate_part) * up_part).astype(jnp.bfloat16))
    for b in range(len(pieces)):
        ready(3 * b + 2)
    for n in range(0, D, COLUMNS):
        total = before_ref[:, n : n + COLUMNS] if carried else None
        for b in range(len(pieces)):
            part = jnp.dot(
                hidden[b], held[3 * b + 2][:, n : n + COLUMNS], preferred_element_type=jnp.float32
            )
            part = part.astype(jnp.bfloat16).astype(jnp.float32)
            total = part if total is None else total + part
        out_ref[:, n : n + COLUMNS] = total.astype(out_ref.dtype)


def experts(rows, blocks, before, after, out_type):
    pieces = [[len(role) for role in block] for block in blocks]
    flat = [piece for block in blocks for role in block for piece in role]
    whole = [
        pltpu.VMEM((len(role) * role[0].shape[0], role[0].shape[1]), jnp.bfloat16)
        for block in blocks
        for role in block
    ]
    count = len(blocks)
    apart = pl.BlockSpec(memory_space=pl.ANY)
    by_rows = pl.BlockSpec((ROWS, D), lambda r: (r, 0))
    operands = [rows, *flat, after]
    in_specs = [by_rows] + [apart] * (len(flat) + 1)
    if before is not None:
        operands.append(before)
        in_specs.append(by_rows)

    def body(*refs):
        experts_kernel(pieces, before is not None, *refs)

    return pl.pallas_call(
        body,
        grid=(rows.shape[0] // ROWS,),
        in_specs=in_specs,
        out_specs=by_rows,
        out_shape=jax.ShapeDtypeStruct(rows.shape, out_type),
        scratch_shapes=whole + [pltpu.SemaphoreType.DMA((len(flat),))],
        compiler_params=pltpu.CompilerParams(dimension_semantics=("arbitrary",)),
        cost_estimate=pl.CostEstimate(
            flops=2 * rows.shape[0] * D * 768 * count,
            bytes_accessed=3_000_000 * count + 12_000_000,
            transcendentals=rows.shape[0] * 256 * count,
        ),
    )(*operands)


def layer(
    q_latent,
    kv_latent,
    rope_key,
    q_gain,
    kv_gain,
    w_query,
    w_query_rot,
    w_key,
    w_value,
    w_mix_out,
    expert_input,
    ffn_gain,
    expert_ids,
    route_weights,
    w_gate_exp,
    w_up_exp,
    w_down_exp,
):
    both = ("ep", "tp")
    tok_rows = q_latent.shape[0]
    ep_count = lax.axis_size("ep")
    tp_count = lax.axis_size("tp")
    group_rows = tp_count * tok_rows
    ep = lax.axis_index("ep")
    tp = lax.axis_index("tp")
    own_start = ep * group_rows + tp * tok_rows

    def shift(by):
        return [
            (e * tp_count + t, e * tp_count + (t + by) % tp_count)
            for e in range(ep_count)
            for t in range(tp_count)
        ]

    mirror = [
        (e * tp_count + t, (ep_count - 1 - e) * tp_count + t)
        for e in range(ep_count)
        for t in range(tp_count)
    ]

    half_rows = tok_rows // 2
    kv_normed = rms_scale(kv_latent, kv_gain).astype(jnp.bfloat16)
    cosine, sine = tables(own_start + jnp.arange(tok_rows, dtype=jnp.int32))
    k_turned = rotate_pairs(rope_key.astype(jnp.float32), cosine, sine).astype(jnp.bfloat16)
    k_packed = jnp.concatenate([k_turned[k * 32 : k * 32 + 32] for k in range(4)], axis=1)
    q_normed = rms_scale(q_latent, q_gain).astype(jnp.bfloat16)
    q_packed = [
        q_normed[half * half_rows : half * half_rows + half_rows, n * 128 : n * 128 + 128]
        for half in range(2)
        for n in range(4)
    ]
    own = jnp.concatenate([kv_normed[:, :128], kv_normed[:, 128:], k_packed, *q_packed], axis=0)
    group = jnp.stack(
        [
            own,
            lax.ppermute(own, both, shift(1)),
            lax.ppermute(own, both, shift(-1)),
            lax.ppermute(own, both, shift(2)),
        ]
    )
    kv_rows = 2 * tok_rows + 32
    kv_all = lax.all_gather(group[:, :kv_rows], "ep", axis=0, tiled=True)
    behind = (jnp.arange(tp_count, dtype=jnp.int32) - tp) % tp_count
    order = jnp.where(behind == 0, 0, jnp.where(behind == 3, 1, jnp.where(behind == 1, 2, 3)))
    place = jnp.concatenate(
        [jnp.stack([ep, jnp.maximum(ep, ep_count - 1 - ep)]), order]
    ).astype(jnp.int32)

    q_mirrored = lax.ppermute(group[:, kv_rows + tok_rows * 2 :], both, mirror)
    q_both = jnp.stack([group[:, kv_rows : kv_rows + tok_rows * 2], q_mirrored])
    spread = (
        jnp.arange(tp_count, dtype=jnp.int32)[:, None] * tok_rows
        + jnp.arange(half_rows, dtype=jnp.int32)[None, :]
    ).reshape(-1)
    q_positions = jnp.concatenate(
        [ep * group_rows + spread, (ep_count - 1 - ep) * group_rows + half_rows + spread]
    )
    q_cosine, q_sine = tables(q_positions)
    q_cosine = q_cosine.reshape(2, QUERIES, ROPE // 2).transpose(0, 2, 1)
    q_sine = q_sine.reshape(2, QUERIES, ROPE // 2).transpose(0, 2, 1)

    gate, up, down = w_gate_exp[0], w_up_exp[0], w_down_exp[0]
    half_units = down.shape[0] // 2
    gate_left = lax.ppermute(gate, both, shift(1))
    gate_right = lax.ppermute(gate, both, shift(-1))
    up_left = lax.ppermute(up, both, shift(1))
    up_right = lax.ppermute(up, both, shift(-1))
    down_left = lax.ppermute(down, both, shift(1))
    down_right = lax.ppermute(down, both, shift(-1))
    gate_across = lax.ppermute(gate_left, both, shift(1))
    up_across = lax.ppermute(up_right, both, shift(-1))
    down_across = [
        lax.ppermute(down_left[:half_units], both, shift(1)),
        lax.ppermute(down_right[half_units:], both, shift(-1)),
    ]

    expert_count = ep_count
    slot_count = 3 * tok_rows * TOPK // (2 * expert_count)
    normed = rms_scale(expert_input, ffn_gain).astype(jnp.bfloat16)
    routed = expert_ids.reshape(-1)
    onehot = (routed[:, None] == jnp.arange(expert_count, dtype=jnp.int32)[None, :]).astype(
        jnp.int32
    )
    slot_number = jnp.sum((jnp.cumsum(onehot, axis=0) - 1) * onehot, axis=-1)
    slot_place = (routed * slot_count + slot_number).reshape(tok_rows, TOPK)
    slot_line = jnp.arange(expert_count * slot_count, dtype=jnp.int32)
    picks = [
        (slot_place[:, route_rank][:, None] == slot_line[None, :]).astype(jnp.bfloat16)
        for route_rank in range(TOPK)
    ]
    dispatch = picks[0]
    for route_rank in range(1, TOPK):
        dispatch = dispatch + picks[route_rank]
    outgoing = lax.dot_general(
        dispatch, normed, BY_FIRST, preferred_element_type=jnp.float32
    ).astype(jnp.bfloat16)
    slot_weights = sum(
        jnp.where(
            slot_place[:, route_rank][:, None] == slot_line[None, :],
            route_weights[:, route_rank : route_rank + 1],
            0.0,
        )
        for route_rank in range(TOPK)
    )
    coarse = slot_weights.astype(jnp.bfloat16)
    fine = (slot_weights - coarse.astype(jnp.float32)).astype(jnp.bfloat16)
    split_weights = jnp.concatenate([coarse, fine], axis=0)
    arrived = lax.all_to_all(
        outgoing.reshape(expert_count, slot_count, D),
        "ep",
        split_axis=0,
        concat_axis=0,
        tiled=True,
    )
    chosen = arrived.reshape(expert_count * slot_count, D)

    near = experts(
        chosen,
        [
            ([gate], [up], [down]),
            ([gate_left], [up_left], [down_left]),
            ([gate_right], [up_right], [down_right]),
        ],
        None,
        place,
        jnp.float32,
    )

    partial_out = attention(
        place,
        kv_all,
        q_both,
        w_query.T,
        w_query_rot.T,
        q_cosine,
        q_sine,
        w_key,
        w_value.T,
        w_mix_out,
        near,
    ).reshape(group_rows, D)
    mixed = lax.psum_scatter(partial_out, "tp", scatter_dimension=0, tiled=True)
    mixer_out = jnp.concatenate(
        [mixed[:half_rows], lax.ppermute(mixed[half_rows:], both, mirror)], axis=0
    )

    results = experts(
        chosen, [([gate_across], [up_across], down_across)], near, partial_out, jnp.bfloat16
    )
    returned = lax.all_to_all(
        results.reshape(expert_count, slot_count, D),
        "ep",
        split_axis=0,
        concat_axis=0,
        tiled=True,
    )
    returned = returned.reshape(expert_count * slot_count, D)

    fetched = jnp.dot(split_weights, returned, preferred_element_type=jnp.float32)
    expert_out = (fetched[:tok_rows] + fetched[tok_rows:]).astype(jnp.bfloat16)
    return (mixer_out, expert_out)


def solution(mesh):
    return jax.shard_map(
        layer,
        mesh=mesh,
        in_specs=(
            P(("ep", "tp"), None),
            P(("ep", "tp"), None),
            P(("ep", "tp"), None),
            P(),
            P(),
            P(None, "tp"),
            P(None, "tp"),
            P(None, "tp"),
            P(None, "tp"),
            P("tp", None),
            P(("ep", "tp"), None),
            P(),
            P(("ep", "tp"), None),
            P(("ep", "tp"), None),
            P("ep", None, "tp"),
            P("ep", None, "tp"),
            P("ep", "tp", None),
        ),
        out_specs=(P(("ep", "tp"), None), P(("ep", "tp"), None)),
        check_vma=False,
    )
```

```python
import math

import jax
import jax.numpy as jnp
from jax import lax
from jax.experimental import pallas as pl
from jax.experimental.pallas import tpu as pltpu
from jax.sharding import PartitionSpec as P


D = 2048
NOPE = 64
ROPE = 32
TOPK = 4

norm_epsilon = 1e-06
rope_base = 10000.0
masked_score = -1e30


KEYS = 512
QUERIES = 256
HEADS_HERE = 4
STEPS_A_CHUNK = 4
PIECE = 256
excess_limit = 60.0
exponent_scale = (NOPE + ROPE) ** (-0.5) * math.log2(math.e)

BY_LAST = (((1,), (1,)), ((), ()))
BY_FIRST = (((0,), (0,)), ((), ()))


def rms_scale(values_in, gain_vec):
    floats = values_in.astype(jnp.float32)
    return (
        floats
        * lax.rsqrt(jnp.mean(floats * floats, axis=-1, keepdims=True) + norm_epsilon)
        * gain_vec
    )


def tables(positions):
    half_width = ROPE // 2
    frequency = rope_base ** (-jnp.arange(half_width, dtype=jnp.float32) / half_width)
    angles = positions.astype(jnp.float32)[:, None] * frequency[None, :]
    return (jnp.cos(angles), jnp.sin(angles))


def rotate_pairs(values_in, cosine, sine_table):
    half_width = values_in.shape[-1] // 2
    first, second = (values_in[..., :half_width], values_in[..., half_width:])
    return jnp.concatenate(
        [first * cosine - second * sine_table, first * sine_table + second * cosine], axis=-1
    )


def attention_kernel(
    place_ref,
    kv_ref,
    q_ref,
    wq_ref,
    wr_ref,
    cos_ref,
    sin_ref,
    wk_ref,
    wv_ref,
    wo_ref,
    after_ref,
    out_ref,
    held_ref,
    query_ref,
    pair_ref,
    vt_ref,
    max_ref,
    sum_ref,
    excess_ref,
    sem,
):
    group = place_ref[0]
    last = place_ref[1]
    low = 31 - last
    chunk = 4 * STEPS_A_CHUNK
    chunks = 32 // STEPS_A_CHUNK
    copies = [
        pltpu.make_async_copy(
            kv_ref.at[pl.ds(n * chunk, chunk)], held_ref.at[pl.ds(n * chunk, chunk)], sem.at[n]
        )
        for n in range(chunks)
    ]
    for copy in copies:
        copy.start()

    for half in range(2):
        rows = jnp.concatenate(
            [
                jnp.concatenate(
                    [
                        q_ref[half, place_ref[2 + t], n * 64 : n * 64 + 64]
                        for n in range(4)
                    ],
                    axis=1,
                )
                for t in range(4)
            ],
            axis=0,
        )
        plain = lax.dot_general(
            wq_ref[...], rows, BY_LAST, preferred_element_type=jnp.float32
        ).astype(jnp.bfloat16)
        turned = lax.dot_general(wr_ref[...], rows, BY_LAST, preferred_element_type=jnp.float32)
        cosine, sine = cos_ref[half], sin_ref[half]
        for h in range(HEADS_HERE):
            first = turned[h * 32 : h * 32 + 16]
            second = turned[h * 32 + 16 : h * 32 + 32]
            at = (h % 2) * 64
            query_ref[half, h, at : at + 64] = plain[h * 64 : h * 64 + 64]
            query_ref[half, h, 64 - at : 128 - at] = jnp.zeros((64, QUERIES), jnp.bfloat16)
            query_ref[half, h, 128:144] = (first * cosine - second * sine).astype(jnp.bfloat16)
            query_ref[half, h, 144:160] = (first * sine + second * cosine).astype(jnp.bfloat16)
            query_ref[half, h, 160:256] = jnp.zeros((96, QUERIES), jnp.bfloat16)
    for h in range(HEADS_HERE):
        vt_ref[h, 64:80] = jnp.ones((16, KEYS), jnp.bfloat16)

    def clear():
        max_ref[...] = jnp.full_like(max_ref, masked_score)
        sum_ref[...] = jnp.zeros_like(sum_ref)

    def project(j):
        base = j * 4
        normed_rows, rope_rows = [], []
        for t in range(4):
            at = base + place_ref[2 + t]
            normed_rows.append(
                jnp.concatenate([held_ref[at, 0:128], held_ref[at, 128:256]], axis=1)
            )
            packed = held_ref[at, 256:288].astype(jnp.float32)
            for k in range(4):
                rope_rows.append(
                    (packed if k == 0 else pltpu.roll(packed, 128 - 32 * k, 1)).astype(jnp.bfloat16)
                )
        normed = jnp.concatenate(normed_rows, axis=0)
        rope = jnp.concatenate(rope_rows, axis=0)
        keys = jnp.dot(normed, wk_ref[...], preferred_element_type=jnp.float32).astype(jnp.bfloat16)
        vals = lax.dot_general(
            wv_ref[...], normed, BY_LAST, preferred_element_type=jnp.float32
        ).astype(jnp.bfloat16)
        for p in range(2):
            pair_ref[p, :, 0:128] = keys[:, p * 128 : p * 128 + 128]
            pair_ref[p, :, 128:256] = rope
        for h in range(HEADS_HERE):
            vt_ref[h, 0:64] = vals[h * 64 : h * 64 + 64]

    def hidden_keys(j, half):
        edge = jnp.where(half == 0, group, 31 - group)
        key_segment = lax.broadcasted_iota(jnp.int32, (KEYS, QUERIES), 0) // 64 + 8 * j
        query_segment = (
            2 * (lax.broadcasted_iota(jnp.int32, (KEYS, QUERIES), 1) // 64) + half + 8 * edge
        )
        return key_segment > query_segment

    def safe_tile(j, half):
        hidden = hidden_keys(j, half)
        for h in range(HEADS_HERE):
            scores = jnp.dot(
                pair_ref[h // 2], query_ref[half, h], preferred_element_type=jnp.float32
            )
            scores = jnp.where(hidden, masked_score, scores)
            old = max_ref[half, h, 0:1]
            new = jnp.maximum(old, jnp.max(scores, axis=0, keepdims=True))
            factor = jnp.exp2((old - new) * exponent_scale)
            weights = jnp.exp2((scores - new) * exponent_scale).astype(jnp.bfloat16)
            part = jnp.dot(vt_ref[h], weights, preferred_element_type=jnp.float32)
            sum_ref[half, h] = sum_ref[half, h] * factor + part
            max_ref[half, h, 0:1] = new

    def tiles(j, halves, masked):
        units = [(half, h) for half in halves for h in range(HEADS_HERE)]
        hidden = hidden_keys(j, halves[0]) if masked else None
        count = len(units)
        base = [max_ref[half, h, 0:1] for half, h in units]
        peak, weights = [None] * count, [None] * count

        def weigh(u):
            half, h = units[u]
            tops, pieces = [], []
            for p in range(0, KEYS, PIECE):
                scores = jnp.dot(
                    pair_ref[h // 2, p : p + PIECE],
                    query_ref[half, h],
                    preferred_element_type=jnp.float32,
                )
                if masked:
                    scores = jnp.where(hidden[p : p + PIECE], masked_score, scores)
                tops.append(jnp.max(scores, axis=0, keepdims=True))
                pieces.append(
                    jnp.exp2((scores - base[u]) * exponent_scale).astype(jnp.bfloat16)
                )
            top = tops[0]
            for other in tops[1:]:
                top = jnp.maximum(top, other)
            peak[u] = top
            weights[u] = jnp.concatenate(pieces, axis=0)

        def gather(u):
            half, h = units[u]
            part = jnp.dot(vt_ref[h], weights[u], preferred_element_type=jnp.float32)
            new = jnp.maximum(base[u], peak[u])
            factor = jnp.exp2((base[u] - new) * exponent_scale)
            sum_ref[half, h] = (sum_ref[half, h] + part) * factor
            max_ref[half, h, 0:1] = new

        for u in range(count + 1):
            if u < count:
                weigh(u)
            if u:
                gather(u - 1)
        most = peak[0] - base[0]
        for u in range(1, count):
            most = jnp.maximum(most, peak[u] - base[u])
        excess_ref[0:1] = jnp.maximum(excess_ref[0:1], most)

    def safe_step(j):
        project(j)
        for half in range(2):
            edge = group if half == 0 else 31 - group

            @pl.when(j <= edge)
            def _():
                safe_tile(j, half)

    def one_half(j):
        for half in range(2):
            edge = group if half == 0 else 31 - group

            @pl.when(jnp.logical_and(j >= low, j < edge))
            def _():
                tiles(j, (half,), False)

            @pl.when(j == edge)
            def _():
                tiles(j, (half,), True)

    clear()
    excess_ref[...] = jnp.zeros_like(excess_ref)
    copies[0].wait()
    lax.fori_loop(0, 1, lambda j, c: (safe_step(j), c)[1], 0)

    def step(j, carried):
        for n in range(1, chunks):

            @pl.when(j == n * STEPS_A_CHUNK)
            def _():
                copies[n].wait()

        project(j)

        @pl.when(j < low)
        def _():
            tiles(j, (0, 1), False)

        @pl.when(j >= low)
        def _():
            one_half(j)

        return carried

    lax.fori_loop(1, last + 1, step, 0)
    for n in range(1, chunks):

        @pl.when(last < n * STEPS_A_CHUNK)
        def _():
            copies[n].wait()

    worst = jnp.max(excess_ref[0:1]) * exponent_scale

    @pl.when(jnp.logical_not(worst < excess_limit))
    def _():
        clear()
        lax.fori_loop(0, last + 1, lambda j, c: (safe_step(j), c)[1], 0)

    for half in range(2):
        heads = [
            (sum_ref[half, h, 0:64] / sum_ref[half, h, 64:65]).astype(jnp.bfloat16)
            for h in range(HEADS_HERE)
        ]
        attended = jnp.concatenate(heads, axis=0)
        part = lax.dot_general(
            attended, wo_ref[...], BY_FIRST, preferred_element_type=jnp.float32
        ).astype(jnp.bfloat16)
        out_ref[:, half] = part.reshape(4, 64, D)


def attention(place, kv, q, wq_t, wr_t, cosine, sine, wk, wv_t, wo, after):
    return pl.pallas_call(
        attention_kernel,
        in_specs=[
            pl.BlockSpec(memory_space=pltpu.SMEM),
            pl.BlockSpec(memory_space=pl.ANY),
        ]
        + [pl.BlockSpec(memory_space=pltpu.VMEM)] * 8
        + [pl.BlockSpec(memory_space=pl.ANY)],
        out_specs=pl.BlockSpec(memory_space=pltpu.VMEM),
        scratch_shapes=[
            pltpu.VMEM((128, 288, 128), jnp.bfloat16),
            pltpu.VMEM((2, HEADS_HERE, 256, QUERIES), jnp.bfloat16),
            pltpu.VMEM((2, KEYS, 256), jnp.bfloat16),
            pltpu.VMEM((HEADS_HERE, 80, KEYS), jnp.bfloat16),
            pltpu.VMEM((2, HEADS_HERE, 8, QUERIES), jnp.float32),
            pltpu.VMEM((2, HEADS_HERE, 80, QUERIES), jnp.float32),
            pltpu.VMEM((8, QUERIES), jnp.float32),
            pltpu.SemaphoreType.DMA((32 // STEPS_A_CHUNK,)),
        ],
        out_shape=jax.ShapeDtypeStruct((4, 2, 64, D), jnp.bfloat16),
        cost_estimate=pl.CostEstimate(
            flops=30_000_000_000, bytes_accessed=16_000_000, transcendentals=17_000_000
        ),
        name="attention",
    )(place, kv, q, wq_t, wr_t, cosine, sine, wk, wv_t, wo, after)


ROWS = 256
COLUMNS = 512
IN_FLIGHT = 4


def experts_kernel(pieces, carried, x_ref, *refs):
    total_pieces = sum(sum(block) for block in pieces)
    parts = refs[:total_pieces]
    refs = refs[total_pieces + 1 :]
    before_ref = None
    if carried:
        before_ref, refs = refs[0], refs[1:]
    out_ref = refs[0]
    held = refs[1 : 1 + 3 * len(pieces)]
    sem = refs[1 + 3 * len(pieces)]
    copies, n = [], 0
    for b, block in enumerate(pieces):
        for role, number in enumerate(block):
            target, own = held[3 * b + role], []
            for piece in range(number):
                rows = target.shape[0] // number
                own.append(
                    pltpu.make_async_copy(
                        parts[n], target.at[pl.ds(piece * rows, rows)], sem.at[n]
                    )
                )
                n += 1
            copies.append(own)
    first_step = pl.program_id(0) == 0
    turn = [n for b in range(len(pieces)) for n in (3 * b, 3 * b + 1)]
    turn = turn + [3 * b + 2 for b in range(len(pieces))]

    @pl.when(first_step)
    def _():
        for n in turn[:IN_FLIGHT]:
            for copy in copies[n]:
                copy.start()

    def ready(n):
        @pl.when(first_step)
        def _():
            for copy in copies[n]:
                copy.wait()
            later = turn.index(n) + IN_FLIGHT
            if later < len(turn):
                for copy in copies[turn[later]]:
                    copy.start()

    rows = x_ref[...]
    hidden = []
    for b in range(len(pieces)):
        ready(3 * b)
        gate_part = jnp.dot(rows, held[3 * b][...], preferred_element_type=jnp.float32)
        ready(3 * b + 1)
        up_part = jnp.dot(rows, held[3 * b + 1][...], preferred_element_type=jnp.float32)
        hidden.append((jax.nn.silu(gate_part) * up_part).astype(jnp.bfloat16))
    for b in range(len(pieces)):
        ready(3 * b + 2)
    for n in range(0, D, COLUMNS):
        total = before_ref[:, n : n + COLUMNS] if carried else None
        for b in range(len(pieces)):
            part = jnp.dot(
                hidden[b], held[3 * b + 2][:, n : n + COLUMNS], preferred_element_type=jnp.float32
            )
            part = part.astype(jnp.bfloat16).astype(jnp.float32)
            total = part if total is None else total + part
        out_ref[:, n : n + COLUMNS] = total.astype(out_ref.dtype)


def experts(rows, blocks, before, after, out_type):
    pieces = [[len(role) for role in block] for block in blocks]
    flat = [piece for block in blocks for role in block for piece in role]
    whole = [
        pltpu.VMEM((len(role) * role[0].shape[0], role[0].shape[1]), jnp.bfloat16)
        for block in blocks
        for role in block
    ]
    count = len(blocks)
    apart = pl.BlockSpec(memory_space=pl.ANY)
    by_rows = pl.BlockSpec((ROWS, D), lambda r: (r, 0))
    operands = [rows, *flat, after]
    in_specs = [by_rows] + [apart] * (len(flat) + 1)
    if before is not None:
        operands.append(before)
        in_specs.append(by_rows)

    def body(*refs):
        experts_kernel(pieces, before is not None, *refs)

    return pl.pallas_call(
        body,
        grid=(rows.shape[0] // ROWS,),
        in_specs=in_specs,
        out_specs=by_rows,
        out_shape=jax.ShapeDtypeStruct(rows.shape, out_type),
        scratch_shapes=whole + [pltpu.SemaphoreType.DMA((len(flat),))],
        compiler_params=pltpu.CompilerParams(dimension_semantics=("arbitrary",)),
        cost_estimate=pl.CostEstimate(
            flops=2 * rows.shape[0] * D * 768 * count,
            bytes_accessed=3_000_000 * count + 12_000_000,
            transcendentals=rows.shape[0] * 256 * count,
        ),
    )(*operands)


def layer(
    q_latent,
    kv_latent,
    rope_key,
    q_gain,
    kv_gain,
    w_query,
    w_query_rot,
    w_key,
    w_value,
    w_mix_out,
    expert_input,
    ffn_gain,
    expert_ids,
    route_weights,
    w_gate_exp,
    w_up_exp,
    w_down_exp,
):
    both = ("ep", "tp")
    tok_rows = q_latent.shape[0]
    ep_count = lax.axis_size("ep")
    tp_count = lax.axis_size("tp")
    group_rows = tp_count * tok_rows
    ep = lax.axis_index("ep")
    tp = lax.axis_index("tp")
    own_start = ep * group_rows + tp * tok_rows

    def shift(by):
        return [
            (e * tp_count + t, e * tp_count + (t + by) % tp_count)
            for e in range(ep_count)
            for t in range(tp_count)
        ]

    mirror = [
        (e * tp_count + t, (ep_count - 1 - e) * tp_count + t)
        for e in range(ep_count)
        for t in range(tp_count)
    ]

    half_rows = tok_rows // 2
    kv_normed = rms_scale(kv_latent, kv_gain).astype(jnp.bfloat16)
    cosine, sine = tables(own_start + jnp.arange(tok_rows, dtype=jnp.int32))
    k_turned = rotate_pairs(rope_key.astype(jnp.float32), cosine, sine).astype(jnp.bfloat16)
    k_packed = jnp.concatenate([k_turned[k * 32 : k * 32 + 32] for k in range(4)], axis=1)
    q_normed = rms_scale(q_latent, q_gain).astype(jnp.bfloat16)
    q_packed = [
        q_normed[half * half_rows : half * half_rows + half_rows, n * 128 : n * 128 + 128]
        for half in range(2)
        for n in range(4)
    ]
    kv_own = jnp.concatenate([kv_normed[:, :128], kv_normed[:, 128:], k_packed], axis=0)
    q_own = jnp.concatenate(q_packed, axis=0)

    def with_neighbours(own):
        return jnp.stack(
            [
                own,
                lax.ppermute(own, both, shift(1)),
                lax.ppermute(own, both, shift(-1)),
                lax.ppermute(own, both, shift(2)),
            ]
        )

    kv_near = with_neighbours(kv_own)
    q_near = with_neighbours(q_own)
    kv_all = lax.all_gather(kv_near, "ep", axis=0, tiled=True)
    behind = (jnp.arange(tp_count, dtype=jnp.int32) - tp) % tp_count
    order = jnp.where(behind == 0, 0, jnp.where(behind == 3, 1, jnp.where(behind == 1, 2, 3)))
    place = jnp.concatenate(
        [jnp.stack([ep, jnp.maximum(ep, ep_count - 1 - ep)]), order]
    ).astype(jnp.int32)

    q_mirrored = lax.ppermute(q_near[:, tok_rows * 2 :], both, mirror)
    q_both = jnp.stack([q_near[:, : tok_rows * 2], q_mirrored])
    spread = (
        jnp.arange(tp_count, dtype=jnp.int32)[:, None] * tok_rows
        + jnp.arange(half_rows, dtype=jnp.int32)[None, :]
    ).reshape(-1)
    q_positions = jnp.concatenate(
        [ep * group_rows + spread, (ep_count - 1 - ep) * group_rows + half_rows + spread]
    )
    q_cosine, q_sine = tables(q_positions)
    q_cosine = q_cosine.reshape(2, QUERIES, ROPE // 2).transpose(0, 2, 1)
    q_sine = q_sine.reshape(2, QUERIES, ROPE // 2).transpose(0, 2, 1)

    gate, up, down = w_gate_exp[0], w_up_exp[0], w_down_exp[0]
    gate_left = lax.ppermute(gate, both, shift(1))
    gate_right = lax.ppermute(gate, both, shift(-1))
    up_left = lax.ppermute(up, both, shift(1))
    up_right = lax.ppermute(up, both, shift(-1))
    down_left = lax.ppermute(down, both, shift(1))
    down_right = lax.ppermute(down, both, shift(-1))
    down_across = lax.ppermute(down, both, shift(2))
    gate_across = lax.ppermute(gate_left, both, shift(1))
    up_across = lax.ppermute(up_left, both, shift(1))

    expert_count = ep_count
    slot_count = 3 * tok_rows * TOPK // (2 * expert_count)
    normed = rms_scale(expert_input, ffn_gain).astype(jnp.bfloat16)
    routed = expert_ids.reshape(-1)
    onehot = (routed[:, None] == jnp.arange(expert_count, dtype=jnp.int32)[None, :]).astype(
        jnp.int32
    )
    slot_number = jnp.sum((jnp.cumsum(onehot, axis=0) - 1) * onehot, axis=-1)
    slot_place = (routed * slot_count + slot_number).reshape(tok_rows, TOPK)
    slot_line = jnp.arange(expert_count * slot_count, dtype=jnp.int32)
    picks = [
        (slot_place[:, route_rank][:, None] == slot_line[None, :]).astype(jnp.bfloat16)
        for route_rank in range(TOPK)
    ]
    dispatch = picks[0]
    for route_rank in range(1, TOPK):
        dispatch = dispatch + picks[route_rank]
    outgoing = lax.dot_general(
        dispatch, normed, BY_FIRST, preferred_element_type=jnp.float32
    ).astype(jnp.bfloat16)
    slot_weights = sum(
        jnp.where(
            slot_place[:, route_rank][:, None] == slot_line[None, :],
            route_weights[:, route_rank : route_rank + 1],
            0.0,
        )
        for route_rank in range(TOPK)
    )
    coarse = slot_weights.astype(jnp.bfloat16)
    fine = (slot_weights - coarse.astype(jnp.float32)).astype(jnp.bfloat16)
    split_weights = jnp.concatenate([coarse, fine], axis=0)
    arrived = lax.all_to_all(
        outgoing.reshape(expert_count, slot_count, D),
        "ep",
        split_axis=0,
        concat_axis=0,
        tiled=True,
    )
    chosen = arrived.reshape(expert_count * slot_count, D)

    partial_out = attention(
        place,
        kv_all,
        q_both,
        w_query.T,
        w_query_rot.T,
        q_cosine,
        q_sine,
        w_key,
        w_value.T,
        w_mix_out,
        place,
    ).reshape(group_rows, D)
    mixed = lax.psum_scatter(partial_out, "tp", scatter_dimension=0, tiled=True)
    mixer_out = jnp.concatenate(
        [mixed[:half_rows], lax.ppermute(mixed[half_rows:], both, mirror)], axis=0
    )

    results = experts(
        chosen,
        [
            ([gate], [up], [down]),
            ([gate_left], [up_left], [down_left]),
            ([gate_right], [up_right], [down_right]),
            ([gate_across], [up_across], [down_across]),
        ],
        None,
        partial_out,
        jnp.bfloat16,
    )
    returned = lax.all_to_all(
        results.reshape(expert_count, slot_count, D),
        "ep",
        split_axis=0,
        concat_axis=0,
        tiled=True,
    )
    returned = returned.reshape(expert_count * slot_count, D)

    fetched = jnp.dot(split_weights, returned, preferred_element_type=jnp.float32)
    expert_out = (fetched[:tok_rows] + fetched[tok_rows:]).astype(jnp.bfloat16)
    return (mixer_out, expert_out)


def solution(mesh):
    return jax.shard_map(
        layer,
        mesh=mesh,
        in_specs=(
            P(("ep", "tp"), None),
            P(("ep", "tp"), None),
            P(("ep", "tp"), None),
            P(),
            P(),
            P(None, "tp"),
            P(None, "tp"),
            P(None, "tp"),
            P(None, "tp"),
            P("tp", None),
            P(("ep", "tp"), None),
            P(),
            P(("ep", "tp"), None),
            P(("ep", "tp"), None),
            P("ep", None, "tp"),
            P("ep", None, "tp"),
            P("ep", "tp", None),
        ),
        out_specs=(P(("ep", "tp"), None), P(("ep", "tp"), None)),
        check_vma=False,
    )
```

```python
import math

import jax
import jax.numpy as jnp
from jax import lax
from jax.experimental import pallas as pl
from jax.experimental.pallas import tpu as pltpu
from jax.sharding import PartitionSpec as P


D = 2048
NOPE = 64
ROPE = 32
TOPK = 4

norm_epsilon = 1e-06
rope_base = 10000.0
masked_score = -1e30


KEYS = 512
QUERIES = 256
HEADS_HERE = 4
STEPS_A_CHUNK = 4
PIECE = 128
excess_limit = 60.0
exponent_scale = (NOPE + ROPE) ** (-0.5) * math.log2(math.e)

BY_LAST = (((1,), (1,)), ((), ()))
BY_FIRST = (((0,), (0,)), ((), ()))


def rms_scale(values_in, gain_vec):
    floats = values_in.astype(jnp.float32)
    return (
        floats
        * lax.rsqrt(jnp.mean(floats * floats, axis=-1, keepdims=True) + norm_epsilon)
        * gain_vec
    )


def tables(positions):
    half_width = ROPE // 2
    frequency = rope_base ** (-jnp.arange(half_width, dtype=jnp.float32) / half_width)
    angles = positions.astype(jnp.float32)[:, None] * frequency[None, :]
    return (jnp.cos(angles), jnp.sin(angles))


def rotate_pairs(values_in, cosine, sine_table):
    half_width = values_in.shape[-1] // 2
    first, second = (values_in[..., :half_width], values_in[..., half_width:])
    return jnp.concatenate(
        [first * cosine - second * sine_table, first * sine_table + second * cosine], axis=-1
    )


def attention_kernel(
    place_ref,
    kv_ref,
    q_ref,
    wq_ref,
    wr_ref,
    cos_ref,
    sin_ref,
    wk_ref,
    wv_ref,
    wo_ref,
    after_ref,
    out_ref,
    held_ref,
    query_ref,
    pair_ref,
    vt_ref,
    max_ref,
    sum_ref,
    excess_ref,
    sem,
):
    group = place_ref[0]
    last = place_ref[1]
    low = 31 - last
    chunk = 4 * STEPS_A_CHUNK
    chunks = 32 // STEPS_A_CHUNK
    copies = [
        pltpu.make_async_copy(
            kv_ref.at[pl.ds(n * chunk, chunk)], held_ref.at[pl.ds(n * chunk, chunk)], sem.at[n]
        )
        for n in range(chunks)
    ]
    for copy in copies:
        copy.start()

    for half in range(2):
        rows = jnp.concatenate(
            [
                jnp.concatenate(
                    [
                        q_ref[half, place_ref[2 + t], n * 64 : n * 64 + 64]
                        for n in range(4)
                    ],
                    axis=1,
                )
                for t in range(4)
            ],
            axis=0,
        )
        plain = lax.dot_general(
            wq_ref[...], rows, BY_LAST, preferred_element_type=jnp.float32
        ).astype(jnp.bfloat16)
        turned = lax.dot_general(wr_ref[...], rows, BY_LAST, preferred_element_type=jnp.float32)
        cosine, sine = cos_ref[half], sin_ref[half]
        for h in range(HEADS_HERE):
            first = turned[h * 32 : h * 32 + 16]
            second = turned[h * 32 + 16 : h * 32 + 32]
            at = (h % 2) * 64
            query_ref[half, h, at : at + 64] = plain[h * 64 : h * 64 + 64]
            query_ref[half, h, 64 - at : 128 - at] = jnp.zeros((64, QUERIES), jnp.bfloat16)
            query_ref[half, h, 128:144] = (first * cosine - second * sine).astype(jnp.bfloat16)
            query_ref[half, h, 144:160] = (first * sine + second * cosine).astype(jnp.bfloat16)
            query_ref[half, h, 160:256] = jnp.zeros((96, QUERIES), jnp.bfloat16)
    for slot in range(2):
        for h in range(HEADS_HERE):
            vt_ref[slot, h, 64:80] = jnp.ones((16, KEYS), jnp.bfloat16)

    def clear():
        max_ref[...] = jnp.full_like(max_ref, masked_score)
        sum_ref[...] = jnp.zeros_like(sum_ref)

    def project(j):
        base = j * 4
        normed_rows, rope_rows = [], []
        for t in range(4):
            at = base + place_ref[2 + t]
            normed_rows.append(
                jnp.concatenate([held_ref[at, 0:128], held_ref[at, 128:256]], axis=1)
            )
            packed = held_ref[at, 256:288].astype(jnp.float32)
            for k in range(4):
                rope_rows.append(
                    (packed if k == 0 else pltpu.roll(packed, 128 - 32 * k, 1)).astype(jnp.bfloat16)
                )
        normed = jnp.concatenate(normed_rows, axis=0)
        rope = jnp.concatenate(rope_rows, axis=0)
        keys = jnp.dot(normed, wk_ref[...], preferred_element_type=jnp.float32).astype(jnp.bfloat16)
        vals = lax.dot_general(
            wv_ref[...], normed, BY_LAST, preferred_element_type=jnp.float32
        ).astype(jnp.bfloat16)

        def store():
            slot = j % 2
            for p in range(2):
                pair_ref[slot, p, :, 0:128] = keys[:, p * 128 : p * 128 + 128]
                pair_ref[slot, p, :, 128:256] = rope
            for h in range(HEADS_HERE):
                vt_ref[slot, h, 0:64] = vals[h * 64 : h * 64 + 64]

        return store

    def hidden_keys(j, half):
        edge = jnp.where(half == 0, group, 31 - group)
        key_segment = lax.broadcasted_iota(jnp.int32, (KEYS, QUERIES), 0) // 64 + 8 * j
        query_segment = (
            2 * (lax.broadcasted_iota(jnp.int32, (KEYS, QUERIES), 1) // 64) + half + 8 * edge
        )
        return key_segment > query_segment

    def safe_tile(j, half):
        hidden = hidden_keys(j, half)
        for h in range(HEADS_HERE):
            scores = jnp.dot(
                pair_ref[j % 2, h // 2], query_ref[half, h], preferred_element_type=jnp.float32
            )
            scores = jnp.where(hidden, masked_score, scores)
            old = max_ref[half, h, 0:1]
            new = jnp.maximum(old, jnp.max(scores, axis=0, keepdims=True))
            factor = jnp.exp2((old - new) * exponent_scale)
            weights = jnp.exp2((scores - new) * exponent_scale).astype(jnp.bfloat16)
            part = jnp.dot(vt_ref[j % 2, h], weights, preferred_element_type=jnp.float32)
            sum_ref[half, h] = sum_ref[half, h] * factor + part
            max_ref[half, h, 0:1] = new

    def tiles(j, halves, masked):
        units = [(half, h) for half in halves for h in range(HEADS_HERE)]
        hidden = hidden_keys(j, halves[0]) if masked else None
        count = len(units)
        base = [max_ref[half, h, 0:1] for half, h in units]
        peak, weights = [None] * count, [None] * count

        def weigh(u):
            half, h = units[u]
            tops, pieces = [], []
            for p in range(0, KEYS, PIECE):
                scores = jnp.dot(
                    pair_ref[j % 2, h // 2, p : p + PIECE],
                    query_ref[half, h],
                    preferred_element_type=jnp.float32,
                )
                if masked:
                    scores = jnp.where(hidden[p : p + PIECE], masked_score, scores)
                tops.append(jnp.max(scores, axis=0, keepdims=True))
                pieces.append(
                    jnp.exp2((scores - base[u]) * exponent_scale).astype(jnp.bfloat16)
                )
            top = tops[0]
            for other in tops[1:]:
                top = jnp.maximum(top, other)
            peak[u] = top
            weights[u] = jnp.concatenate(pieces, axis=0)

        def gather(u):
            half, h = units[u]
            part = jnp.dot(vt_ref[j % 2, h], weights[u], preferred_element_type=jnp.float32)
            new = jnp.maximum(base[u], peak[u])
            factor = jnp.exp2((base[u] - new) * exponent_scale)
            sum_ref[half, h] = (sum_ref[half, h] + part) * factor
            max_ref[half, h, 0:1] = new

        store = project(jnp.minimum(j + 1, 31))
        for u in range(count + 1):
            if u < count:
                weigh(u)
            if u:
                gather(u - 1)
        store()
        most = peak[0] - base[0]
        for u in range(1, count):
            most = jnp.maximum(most, peak[u] - base[u])
        excess_ref[0:1] = jnp.maximum(excess_ref[0:1], most)

    def safe_step(j):
        project(j)()

        def one(half, carried):
            @pl.when(j <= jnp.where(half == 0, group, 31 - group))
            def _():
                safe_tile(j, half)

            return carried

        lax.fori_loop(0, 2, one, 0)

    def one_half(j):
        for half in range(2):
            edge = group if half == 0 else 31 - group

            @pl.when(jnp.logical_and(j >= low, j < edge))
            def _():
                tiles(j, (half,), False)

        @pl.when(jnp.logical_or(j == group, j == 31 - group))
        def _():
            tiles(j, (jnp.where(j == group, 0, 1),), True)

    def step(j, carried):
        for n in range(1, chunks):

            @pl.when(j + 1 == n * STEPS_A_CHUNK)
            def _():
                copies[n].wait()

        @pl.when(j < low)
        def _():
            tiles(j, (0, 1), False)

        @pl.when(j >= low)
        def _():
            one_half(j)

        return carried

    def attempt(again, carried):
        worst = jnp.max(excess_ref[0:1]) * exponent_scale
        redo = jnp.logical_and(again == 1, jnp.logical_not(worst < excess_limit))

        @pl.when(jnp.logical_or(again == 0, redo))
        def _():
            clear()

        safe_steps = jnp.where(again == 0, 1, jnp.where(redo, last + 1, 0))
        lax.fori_loop(0, safe_steps, lambda j, c: (safe_step(j), c)[1], 0)

        @pl.when(again == 0)
        def _():
            project(1)()

        lax.fori_loop(1, jnp.where(again == 0, last + 1, 1), step, 0)
        return carried

    excess_ref[...] = jnp.zeros_like(excess_ref)
    copies[0].wait()
    lax.fori_loop(0, 2, attempt, 0)
    for n in range(1, chunks):

        @pl.when(last + 1 < n * STEPS_A_CHUNK)
        def _():
            copies[n].wait()

    for half in range(2):
        heads = [
            (sum_ref[half, h, 0:64] / sum_ref[half, h, 64:65]).astype(jnp.bfloat16)
            for h in range(HEADS_HERE)
        ]
        attended = jnp.concatenate(heads, axis=0)
        part = lax.dot_general(
            attended, wo_ref[...], BY_FIRST, preferred_element_type=jnp.float32
        ).astype(jnp.bfloat16)
        out_ref[:, half] = part.reshape(4, 64, D)


def attention(place, kv, q, wq_t, wr_t, cosine, sine, wk, wv_t, wo, after):
    return pl.pallas_call(
        attention_kernel,
        in_specs=[
            pl.BlockSpec(memory_space=pltpu.SMEM),
            pl.BlockSpec(memory_space=pl.ANY),
        ]
        + [pl.BlockSpec(memory_space=pltpu.VMEM)] * 8
        + [pl.BlockSpec(memory_space=pl.ANY)],
        out_specs=pl.BlockSpec(memory_space=pltpu.VMEM),
        scratch_shapes=[
            pltpu.VMEM((128, 288, 128), jnp.bfloat16),
            pltpu.VMEM((2, HEADS_HERE, 256, QUERIES), jnp.bfloat16),
            pltpu.VMEM((2, 2, KEYS, 256), jnp.bfloat16),
            pltpu.VMEM((2, HEADS_HERE, 80, KEYS), jnp.bfloat16),
            pltpu.VMEM((2, HEADS_HERE, 8, QUERIES), jnp.float32),
            pltpu.VMEM((2, HEADS_HERE, 80, QUERIES), jnp.float32),
            pltpu.VMEM((8, QUERIES), jnp.float32),
            pltpu.SemaphoreType.DMA((32 // STEPS_A_CHUNK,)),
        ],
        out_shape=jax.ShapeDtypeStruct((4, 2, 64, D), jnp.bfloat16),
        cost_estimate=pl.CostEstimate(
            flops=30_000_000_000, bytes_accessed=16_000_000, transcendentals=17_000_000
        ),
        name="attention",
    )(place, kv, q, wq_t, wr_t, cosine, sine, wk, wv_t, wo, after)


ROWS = 768
COLUMNS = 512
IN_FLIGHT = 4


def experts_kernel(pieces, carried, x_ref, *refs):
    total_pieces = sum(sum(block) for block in pieces)
    parts = refs[:total_pieces]
    refs = refs[total_pieces + 1 :]
    before_ref = None
    if carried:
        before_ref, refs = refs[0], refs[1:]
    out_ref = refs[0]
    held = refs[1 : 1 + 3 * len(pieces)]
    sem = refs[1 + 3 * len(pieces)]
    copies, n = [], 0
    for b, block in enumerate(pieces):
        for role, number in enumerate(block):
            target, own = held[3 * b + role], []
            for piece in range(number):
                rows = target.shape[0] // number
                own.append(
                    pltpu.make_async_copy(
                        parts[n], target.at[pl.ds(piece * rows, rows)], sem.at[n]
                    )
                )
                n += 1
            copies.append(own)
    first_step = pl.program_id(0) == 0
    turn = [n for b in range(len(pieces)) for n in (3 * b, 3 * b + 1)]
    turn = turn + [3 * b + 2 for b in range(len(pieces))]

    @pl.when(first_step)
    def _():
        for n in turn[:IN_FLIGHT]:
            for copy in copies[n]:
                copy.start()

    def ready(n):
        @pl.when(first_step)
        def _():
            for copy in copies[n]:
                copy.wait()
            later = turn.index(n) + IN_FLIGHT
            if later < len(turn):
                for copy in copies[turn[later]]:
                    copy.start()

    rows = x_ref[...]
    hidden = []
    for b in range(len(pieces)):
        ready(3 * b)
        gate_part = jnp.dot(rows, held[3 * b][...], preferred_element_type=jnp.float32)
        ready(3 * b + 1)
        up_part = jnp.dot(rows, held[3 * b + 1][...], preferred_element_type=jnp.float32)
        hidden.append((jax.nn.silu(gate_part) * up_part).astype(jnp.bfloat16))
    for b in range(len(pieces)):
        ready(3 * b + 2)
    for n in range(0, D, COLUMNS):
        total = before_ref[:, n : n + COLUMNS] if carried else None
        for b in range(len(pieces)):
            part = jnp.dot(
                hidden[b], held[3 * b + 2][:, n : n + COLUMNS], preferred_element_type=jnp.float32
            )
            part = part.astype(jnp.bfloat16).astype(jnp.float32)
            total = part if total is None else total + part
        out_ref[:, n : n + COLUMNS] = total.astype(out_ref.dtype)


def experts(rows, blocks, before, after, out_type):
    pieces = [[len(role) for role in block] for block in blocks]
    flat = [piece for block in blocks for role in block for piece in role]
    whole = [
        pltpu.VMEM((len(role) * role[0].shape[0], role[0].shape[1]), jnp.bfloat16)
        for block in blocks
        for role in block
    ]
    count = len(blocks)
    apart = pl.BlockSpec(memory_space=pl.ANY)
    by_rows = pl.BlockSpec((ROWS, D), lambda r: (r, 0))
    operands = [rows, *flat, after]
    in_specs = [by_rows] + [apart] * (len(flat) + 1)
    if before is not None:
        operands.append(before)
        in_specs.append(by_rows)

    def body(*refs):
        experts_kernel(pieces, before is not None, *refs)

    return pl.pallas_call(
        body,
        grid=(rows.shape[0] // ROWS,),
        in_specs=in_specs,
        out_specs=by_rows,
        out_shape=jax.ShapeDtypeStruct(rows.shape, out_type),
        scratch_shapes=whole + [pltpu.SemaphoreType.DMA((len(flat),))],
        compiler_params=pltpu.CompilerParams(dimension_semantics=("arbitrary",)),
        cost_estimate=pl.CostEstimate(
            flops=2 * rows.shape[0] * D * 768 * count,
            bytes_accessed=3_000_000 * count + 12_000_000,
            transcendentals=rows.shape[0] * 256 * count,
        ),
    )(*operands)


def layer(
    q_latent,
    kv_latent,
    rope_key,
    q_gain,
    kv_gain,
    w_query,
    w_query_rot,
    w_key,
    w_value,
    w_mix_out,
    expert_input,
    ffn_gain,
    expert_ids,
    route_weights,
    w_gate_exp,
    w_up_exp,
    w_down_exp,
):
    both = ("ep", "tp")
    tok_rows = q_latent.shape[0]
    ep_count = lax.axis_size("ep")
    tp_count = lax.axis_size("tp")
    group_rows = tp_count * tok_rows
    ep = lax.axis_index("ep")
    tp = lax.axis_index("tp")
    own_start = ep * group_rows + tp * tok_rows

    def shift(by):
        return [
            (e * tp_count + t, e * tp_count + (t + by) % tp_count)
            for e in range(ep_count)
            for t in range(tp_count)
        ]

    mirror = [
        (e * tp_count + t, (ep_count - 1 - e) * tp_count + t)
        for e in range(ep_count)
        for t in range(tp_count)
    ]

    half_rows = tok_rows // 2
    kv_normed = rms_scale(kv_latent, kv_gain).astype(jnp.bfloat16)
    cosine, sine = tables(own_start + jnp.arange(tok_rows, dtype=jnp.int32))
    k_turned = rotate_pairs(rope_key.astype(jnp.float32), cosine, sine).astype(jnp.bfloat16)
    k_packed = jnp.concatenate([k_turned[k * 32 : k * 32 + 32] for k in range(4)], axis=1)
    q_normed = rms_scale(q_latent, q_gain).astype(jnp.bfloat16)
    q_packed = [
        q_normed[half * half_rows : half * half_rows + half_rows, n * 128 : n * 128 + 128]
        for half in range(2)
        for n in range(4)
    ]
    kv_own = jnp.concatenate([kv_normed[:, :128], kv_normed[:, 128:], k_packed], axis=0)
    q_own = jnp.concatenate(q_packed, axis=0)

    def with_neighbours(own):
        return jnp.stack(
            [
                own,
                lax.ppermute(own, both, shift(1)),
                lax.ppermute(own, both, shift(-1)),
                lax.ppermute(own, both, shift(2)),
            ]
        )

    kv_near = with_neighbours(kv_own)
    q_near = with_neighbours(q_own)
    kv_all = lax.all_gather(kv_near, "ep", axis=0, tiled=True)
    behind = (jnp.arange(tp_count, dtype=jnp.int32) - tp) % tp_count
    order = jnp.where(behind == 0, 0, jnp.where(behind == 3, 1, jnp.where(behind == 1, 2, 3)))
    place = jnp.concatenate(
        [jnp.stack([ep, jnp.maximum(ep, ep_count - 1 - ep)]), order]
    ).astype(jnp.int32)

    q_mirrored = lax.ppermute(q_near[:, tok_rows * 2 :], both, mirror)
    q_both = jnp.stack([q_near[:, : tok_rows * 2], q_mirrored])
    spread = (
        jnp.arange(tp_count, dtype=jnp.int32)[:, None] * tok_rows
        + jnp.arange(half_rows, dtype=jnp.int32)[None, :]
    ).reshape(-1)
    q_positions = jnp.concatenate(
        [ep * group_rows + spread, (ep_count - 1 - ep) * group_rows + half_rows + spread]
    )
    q_cosine, q_sine = tables(q_positions)
    q_cosine = q_cosine.reshape(2, QUERIES, ROPE // 2).transpose(0, 2, 1)
    q_sine = q_sine.reshape(2, QUERIES, ROPE // 2).transpose(0, 2, 1)

    gate, up, down = w_gate_exp[0], w_up_exp[0], w_down_exp[0]
    half_units = down.shape[0] // 2
    gate_left = lax.ppermute(gate, both, shift(1))
    gate_right = lax.ppermute(gate, both, shift(-1))
    up_left = lax.ppermute(up, both, shift(1))
    up_right = lax.ppermute(up, both, shift(-1))
    down_top, down_low = down[:half_units], down[half_units:]
    top_left = lax.ppermute(down_top, both, shift(1))
    low_right = lax.ppermute(down_low, both, shift(-1))
    low_left = lax.ppermute(down_low, both, shift(1))
    top_right = lax.ppermute(down_top, both, shift(-1))
    top_across = lax.ppermute(top_left, both, shift(1))
    low_across = lax.ppermute(low_right, both, shift(-1))
    gate_across = lax.ppermute(gate_left, both, shift(1))
    up_across = lax.ppermute(up_right, both, shift(-1))

    expert_count = ep_count
    slot_count = 3 * tok_rows * TOPK // (2 * expert_count)
    normed = rms_scale(expert_input, ffn_gain).astype(jnp.bfloat16)
    routed = expert_ids.reshape(-1)
    onehot = (routed[:, None] == jnp.arange(expert_count, dtype=jnp.int32)[None, :]).astype(
        jnp.int32
    )
    slot_number = jnp.sum((jnp.cumsum(onehot, axis=0) - 1) * onehot, axis=-1)
    slot_place = (routed * slot_count + slot_number).reshape(tok_rows, TOPK)
    slot_line = jnp.arange(expert_count * slot_count, dtype=jnp.int32)
    picks = [
        (slot_place[:, route_rank][:, None] == slot_line[None, :]).astype(jnp.bfloat16)
        for route_rank in range(TOPK)
    ]
    dispatch = picks[0]
    for route_rank in range(1, TOPK):
        dispatch = dispatch + picks[route_rank]
    outgoing = lax.dot_general(
        dispatch, normed, BY_FIRST, preferred_element_type=jnp.float32
    ).astype(jnp.bfloat16)
    slot_weights = sum(
        jnp.where(
            slot_place[:, route_rank][:, None] == slot_line[None, :],
            route_weights[:, route_rank : route_rank + 1],
            0.0,
        )
        for route_rank in range(TOPK)
    )
    coarse = slot_weights.astype(jnp.bfloat16)
    fine = (slot_weights - coarse.astype(jnp.float32)).astype(jnp.bfloat16)
    split_weights = jnp.concatenate([coarse, fine], axis=0)
    arrived = lax.all_to_all(
        outgoing.reshape(expert_count, slot_count, D),
        "ep",
        split_axis=0,
        concat_axis=0,
        tiled=True,
    )
    chosen = arrived.reshape(expert_count * slot_count, D)

    partial_out = attention(
        place,
        kv_all,
        q_both,
        w_query.T,
        w_query_rot.T,
        q_cosine,
        q_sine,
        w_key,
        w_value.T,
        w_mix_out,
        place,
    ).reshape(group_rows, D)
    mixed = lax.psum_scatter(partial_out, "tp", scatter_dimension=0, tiled=True)
    mixer_out = jnp.concatenate(
        [mixed[:half_rows], lax.ppermute(mixed[half_rows:], both, mirror)], axis=0
    )

    results = experts(
        chosen,
        [
            ([gate], [up], [down]),
            ([gate_left], [up_left], [top_left, low_left]),
            ([gate_right], [up_right], [top_right, low_right]),
            ([gate_across], [up_across], [top_across, low_across]),
        ],
        None,
        partial_out,
        jnp.bfloat16,
    )
    returned = lax.all_to_all(
        results.reshape(expert_count, slot_count, D),
        "ep",
        split_axis=0,
        concat_axis=0,
        tiled=True,
    )
    returned = returned.reshape(expert_count * slot_count, D)

    fetched = jnp.dot(split_weights, returned, preferred_element_type=jnp.float32)
    expert_out = (fetched[:tok_rows] + fetched[tok_rows:]).astype(jnp.bfloat16)
    return (mixer_out, expert_out)


def solution(mesh):
    return jax.shard_map(
        layer,
        mesh=mesh,
        in_specs=(
            P(("ep", "tp"), None),
            P(("ep", "tp"), None),
            P(("ep", "tp"), None),
            P(),
            P(),
            P(None, "tp"),
            P(None, "tp"),
            P(None, "tp"),
            P(None, "tp"),
            P("tp", None),
            P(("ep", "tp"), None),
            P(),
            P(("ep", "tp"), None),
            P(("ep", "tp"), None),
            P("ep", None, "tp"),
            P("ep", None, "tp"),
            P("ep", "tp", None),
        ),
        out_specs=(P(("ep", "tp"), None), P(("ep", "tp"), None)),
        check_vma=False,
    )
```
